32 devices in a mesh: gr: 2 (over core), fs: 8 (over z, y), tp: 2 (over x).
Axes of the slice: x: 2, y: 2, z: 4, core: 2. Of those that a mesh axis runs over, the one named last changes fastest.
Arguments:
- prompt: bfloat16 [5120, 2048], P(('gr', 'fs'), 'tp'), may hold values from -6 to 6
- norm_gain: float32 [2048], P(('gr', 'fs')), may hold values from 0.1 to 1.9
- gate_weight: float32 [32, 2048, 2048], P(None, ('gr', 'fs'), 'tp'), may hold values from -0.125 to 0.125
- up_weight: float32 [32, 2048, 2048], P(None, ('gr', 'fs'), 'tp'), may hold values from -0.125 to 0.125
- down_weight: float32 [32, 2048, 2048], P(None, ('gr', 'fs'), 'tp'), may hold values from -0.125 to 0.125
- routes: int32 [5120, 2], P(('gr', 'fs')), may hold values from 0 to 31, as said below
- route_weight: float32 [5120, 2], P(('gr', 'fs')), may hold values from 0.2 to 1
Outputs:
- gate_new: bfloat16 [32, 2048, 2048], P('fs', None, 'tp')
- up_new: bfloat16 [32, 2048, 2048], P('fs', None, 'tp')
- down_new: bfloat16 [32, 2048, 2048], P('fs', 'tp')
- mixed: bfloat16 [5120, 2048], P(('gr', 'fs'), 'tp')
The draws below stay inside these ranges and needn't reach their ends.
Inputs may be any that keep to these rules, and one draw needn't show every extreme that they name: `routes`: each row names two different experts of the same group; expert e belongs to group e // 8. Among the 320 rows of one index of gr and fs no expert is named more than 30 times, and in every draw every expert of one group is named exactly 30 times by the rows of every index.
All inputs are finite; a program needn't handle non-finite values.
Results may differ from the reference program's by a relative error of at most 0.015.
Values may be sent and summed in bfloat16 or wider, within the bound.
A program may use at most 256 MiB of HBM per device.

```python
import jax
import jax.numpy as jnp
from jax import lax

D = 2048
FF = 2048
GROUPS = 4
EXP_GROUP = 8
TOK_DEV = 320
EXPERTS = 32
CAP = 30
TOKENS = 5120
N_GR = 2
N_FS = 8
N_TP = 2


def draw_routes(key, part):
    big_group = jax.random.randint(jax.random.fold_in(key, 101), (), 0, GROUPS)
    full = 4 * CAP
    rest = TOK_DEV - full
    spacing = rest // (GROUPS - 1)
    jitter = spacing // 4

    def one_source(source):
        source_key = jax.random.fold_in(key, source)
        key_rank, key_bound, key_shift = jax.random.split(source_key, 3)
        ranking = jax.random.permutation(key_rank, TOK_DEV).astype(jnp.int32)
        inner = jnp.arange(1, GROUPS - 1, dtype=jnp.int32) * rest // (GROUPS - 1)
        inner = inner + jax.random.randint(key_bound, (GROUPS - 2,), -jitter, jitter + 1)
        bounds = jnp.concatenate([jnp.zeros((1,), jnp.int32), inner.astype(jnp.int32)])
        remain = ranking - full
        slot_index = jnp.sum((remain[:, None] >= inner[None, :]).astype(jnp.int32), axis=1)
        in_big = ranking < full
        within = jnp.where(in_big, ranking, remain - bounds[slot_index])
        other = slot_index + (slot_index >= big_group).astype(jnp.int32)
        group_id = jnp.where(in_big, big_group, other)
        shifts = jax.random.randint(key_shift, (GROUPS,), 0, EXP_GROUP)
        offset = shifts[group_id]
        first = (within + offset) % EXP_GROUP
        second = (within + offset + 1 + within // EXP_GROUP % (EXP_GROUP - 1)) % EXP_GROUP
        return jnp.stack([group_id * EXP_GROUP + first, group_id * EXP_GROUP + second], axis=1)
    sources = jnp.arange(N_GR * N_FS, dtype=jnp.int32)
    return jax.vmap(one_source)(sources).reshape(TOKENS, 2).astype(jnp.int32)


def level_of(key, extent, shards, low, top_value):
    gain, own = 1.0, jax.random.fold_in(key, 6)
    for position, shards_of in shards:
        steps = jnp.exp(jax.random.uniform(jax.random.fold_in(own, position), (shards_of,), jnp.float32, low / len(shards), top_value / len(shards)))
        gain = gain * jnp.repeat(steps, extent[position] // shards_of).reshape([-1 if axis == position else 1 for axis in range(len(extent))])
    return gain


def normal_values(rng, shape, width, most, cuts=(), held_as=jnp.bfloat16):
    drawn = jax.random.normal(rng, shape, jnp.float32) * width
    if len(cuts) > 0:
        drawn = level_of(rng, shape, cuts, -0.22, 0.18) * drawn
    return jnp.clip(drawn, min=-most, max=most).astype(held_as)


def setup_inputs(seed: int = 0) -> dict:
    streams_of = jax.random.split(jax.random.key(seed), 8)
    return {
        "prompt": normal_values(streams_of[0], (TOKENS, D), 1.0, 6.0, ((0, 16), (1, 2))),
        "norm_gain": jnp.clip(1.0 + 0.18 * jax.random.normal(streams_of[1], (D,), jnp.float32), 0.1, 1.9),
        "gate_weight": normal_values(streams_of[2], (EXPERTS, D, FF), D ** -0.5, 0.125, ((1, 16), (2, 2)), jnp.float32),
        "up_weight": normal_values(streams_of[3], (EXPERTS, D, FF), D ** -0.5, 0.125, ((1, 16), (2, 2)), jnp.float32),
        "down_weight": normal_values(streams_of[4], (EXPERTS, FF, D), FF ** -0.5, 0.125, ((1, 16), (2, 2)), jnp.float32),
        "routes": draw_routes(jax.random.fold_in(streams_of[7], 71), 0),
        "route_weight": jnp.clip(0.2 + 0.8 * jax.random.uniform(streams_of[6], (TOKENS, 2), jnp.float32) ** level_of(streams_of[6], (TOKENS, 2), ((0, 16),), -0.2, 0.2), 0.2, 1.0),
    }


def reference(prompt, norm_gain, gate_weight, up_weight, down_weight, routes, route_weight):
    gate_new = (gate_weight * norm_gain[None, :, None]).astype(jnp.bfloat16)
    up_new = (up_weight * norm_gain[None, :, None]).astype(jnp.bfloat16)
    down_new = down_weight.astype(jnp.bfloat16)
    values = prompt.astype(jnp.float32)
    normed = (values * lax.rsqrt(lax.optimization_barrier(jnp.mean(values * values, axis=-1, keepdims=True)) + 1e-06)).astype(jnp.bfloat16)
    picks_flat = routes.reshape(-1)
    total = picks_flat.shape[0]
    most = N_GR * N_FS * CAP
    normed_pad = jnp.concatenate([normed, jnp.zeros((1, D), jnp.bfloat16)], axis=0)
    weight_pad = jnp.concatenate([route_weight.reshape(-1), jnp.zeros((1,), jnp.float32)], axis=0)

    def one_expert(accum, expert):
        chosen = jnp.nonzero(picks_flat == expert, size=most, fill_value=total)[0].astype(jnp.int32)
        tok_rows = (chosen // 2).astype(jnp.int32)
        arrived = normed_pad[tok_rows]
        gate_pre = jnp.dot(arrived, gate_new[expert], preferred_element_type=jnp.float32)
        up_pre = jnp.dot(arrived, up_new[expert], preferred_element_type=jnp.float32)
        hidden = (jax.nn.silu(gate_pre) * up_pre).astype(jnp.bfloat16)
        blocks = hidden.reshape(most, N_TP, FF // N_TP).astype(jnp.float32)
        down_blocks = down_new[expert].reshape(N_TP, FF // N_TP, D).astype(jnp.float32)
        partial_value = jnp.einsum('rkh,khd->rkd', blocks, down_blocks).astype(jnp.bfloat16)
        partial_value = lax.optimization_barrier(partial_value).astype(jnp.float32)
        expert_out = lax.optimization_barrier(jnp.sum(partial_value, axis=1)).astype(jnp.bfloat16)
        expert_out = lax.optimization_barrier(expert_out).astype(jnp.float32)
        accum = accum.at[tok_rows].add(expert_out * weight_pad[chosen][:, None])
        return (accum, None)
    start = jnp.zeros((TOKENS + 1, D), jnp.float32)
    accum, _ = lax.scan(one_expert, start, jnp.arange(EXPERTS, dtype=jnp.int32))
    mixed = accum[:TOKENS].astype(jnp.bfloat16)
    return (gate_new, up_new, down_new, mixed)
```

```python
import functools

import jax
import jax.numpy as jnp
from jax import lax
from jax.experimental import pallas as pl
from jax.experimental.pallas import tpu as pltpu
from jax.sharding import PartitionSpec as P

CAP = 30
SLOT = -(-CAP // 16) * 16
MESH = pl.DeviceIdType.MESH


def remote(src, dst, send, recv, device):
    copy = pltpu.make_async_remote_copy(
        src_ref=src, dst_ref=dst, send_sem=send, recv_sem=recv, device_id=device, device_id_type=MESH
    )
    copy.start()


def settle(ref, sem):
    pltpu.make_async_copy(ref, ref, sem).wait()


def loop(low, high, step):
    lax.fori_loop(low, high, lambda index, carry: (step(index), carry)[1], 0)


def span(index, size):
    return pl.ds(pl.multiple_of(index * size, size), size)


def greet(barrier, device):
    pl.semaphore_signal(barrier, inc=1, device_id=device, device_id_type=MESH)


def spread_kernel(
    sizes, tok, gate, up, down, arr, gate_out, up_out, down_out,
    own_tok, own, tok_send, tok_recv, share_send, share_recv,
    w_send, w_recv, twin_send, twin_recv, own_sem,
):
    n_gr, n_fs, n_tp = sizes
    gr, fs, tp = lax.axis_index("gr"), lax.axis_index("fs"), lax.axis_index("tp")
    per, blk, wide = gate_out.shape[0], gate.shape[1], gate.shape[2]
    per_tp = n_gr * n_fs // n_tp
    row = gr * n_fs + fs
    owner = row // per_tp
    home = tp * per_tp // n_fs
    ring = n_fs * n_tp

    barrier = pltpu.get_barrier_semaphore()

    def greet_plane(k):
        other = (fs * n_tp + tp + k) % ring
        greet(barrier, (gr, other // n_tp, other % n_tp))

    loop(1, ring, greet_plane)
    loop(1, n_gr, lambda k: greet(barrier, ((gr + k) % n_gr, fs, tp)))
    pl.semaphore_wait(barrier, ring + n_gr - 2)

    def tok_place(source, t):
        return arr.at[:, source, :, span(t, wide)]

    def rows_of(out, index):
        return out.at[:, span(index, blk), :]

    def down_place(index):
        return down_out.at[:, span(index, blk), span(tp, wide)]

    def mine(ref, f):
        return ref.at[pl.ds(f * per, per)]

    loads = [pltpu.make_async_copy(tok.at[fs], own_tok, own_sem.at[3])]
    for w, ref in enumerate((gate, up, down)):
        loads.append(pltpu.make_async_copy(mine(ref, fs), own.at[w], own_sem.at[w]))
    for load in loads:
        load.start()

    def far(k):
        return (fs + (k + n_fs // 2 - 1) % (n_fs - 1) + 1) % n_fs

    def send_tok(k):
        f = far(k)
        remote(tok.at[f], tok_place(fs, tp), tok_send, tok_recv.at[fs], (gr, f, tp))

    loop(0, n_fs - 1, send_tok)

    def send_down(k):
        f = far(k)
        remote(mine(down, f), down_place(row - owner * per_tp), w_send.at[2], w_recv.at[2, fs], (gr, f, owner))

    loop(0, n_fs - 1, send_down)
    for w, (ref, out) in enumerate(((gate, gate_out), (up, up_out))):

        def send_w(k, w=w, ref=ref, out=out):
            f = far(k)
            remote(mine(ref, f), rows_of(out, row), w_send.at[w], w_recv.at[w, fs], (gr, f, tp))

        loop(0, n_fs - 1, send_w)

    for load in loads:
        load.wait()
    pltpu.make_async_copy(own_tok, tok_place(fs, tp), tok_recv.at[fs]).start()
    pltpu.make_async_copy(own.at[0], rows_of(gate_out, row), w_recv.at[0, fs]).start()
    pltpu.make_async_copy(own.at[1], rows_of(up_out, row), w_recv.at[1, fs]).start()

    @pl.when(owner == tp)
    def _():
        pltpu.make_async_copy(own.at[2], down_place(row - owner * per_tp), w_recv.at[2, fs]).start()

    @pl.when(owner != tp)
    def _():
        remote(own.at[2], down_place(row - owner * per_tp), w_send.at[2], w_recv.at[2, fs], (gr, fs, owner))

    def share_tok(k):
        source = (fs + n_fs - k) % n_fs
        place = tok_place(source, tp)
        settle(place, tok_recv.at[source])
        for j in range(1, n_tp):
            t = (tp + j) % n_tp
            remote(place, place, share_send.at[t], share_recv.at[tp], (gr, fs, t))

    loop(0, n_fs, share_tok)

    @pl.when(home == gr)
    def _():
        def twin_down(k):
            source = tp * per_tp - gr * n_fs + k
            place = rows_of(down_out, k)
            settle(place, w_recv.at[2, source])
            for j in range(1, n_gr):
                g = (gr + j) % n_gr
                remote(place, place, twin_send.at[2, g], twin_recv.at[2, gr], (g, fs, tp))

        loop(0, per_tp, twin_down)

    for w, out in enumerate((gate_out, up_out)):

        def twin_w(k, w=w, out=out):
            source = (fs + n_fs - k) % n_fs
            place = rows_of(out, gr * n_fs + source)
            settle(place, w_recv.at[w, source])
            for j in range(1, n_gr):
                g = (gr + j) % n_gr
                remote(place, place, twin_send.at[w, g], twin_recv.at[w, gr], (g, fs, tp))

        loop(0, n_fs, twin_w)

    settle(tok.at[pl.ds(0, n_fs - 1)], tok_send)
    for w, ref in enumerate((gate, up)):
        settle(ref.at[pl.ds(0, (n_fs - 1) * per)], w_send.at[w])

    @pl.when(owner == tp)
    def _():
        settle(down.at[pl.ds(0, (n_fs - 1) * per)], w_send.at[2])

    @pl.when(owner != tp)
    def _():
        settle(down, w_send.at[2])

    for j in range(1, n_tp):
        t = (tp + j) % n_tp
        settle(arr.at[:, :, :, span(tp, wide)], share_send.at[t])
        settle(arr.at[:, :, :, span(t, wide)], share_recv.at[t])
    for j in range(1, n_gr):
        g = (gr + j) % n_gr
        for w, out in enumerate((gate_out, up_out)):
            settle(out.at[:, span(gr, n_fs * blk), :], twin_send.at[w, g])
            settle(out.at[:, span(g, n_fs * blk), :], twin_recv.at[w, g])

        @pl.when(home == gr)
        def _():
            settle(down_out, twin_send.at[2, g])

    @pl.when(home != gr)
    def _():
        settle(down_out, twin_recv.at[2, home])


def return_kernel(sizes, part, ret, got, summed, x_send, x_recv, z_send, z_recv):
    n_gr, n_fs, n_tp = sizes
    gr, fs, tp = lax.axis_index("gr"), lax.axis_index("fs"), lax.axis_index("tp")
    per, wide = part.shape[0], ret.shape[3]

    barrier = pltpu.get_barrier_semaphore()
    loop(1, n_fs, lambda k: greet(barrier, (gr, (fs + k) % n_fs, tp)))
    loop(1, n_tp, lambda k: greet(barrier, (gr, fs, (tp + k) % n_tp)))
    pl.semaphore_wait(barrier, n_fs + n_tp - 2)

    def exchange(x):
        for j in range(1, n_tp):
            t = (tp + j) % n_tp
            remote(part.at[x, :, :, span(t, wide)], got.at[tp, x], x_send.at[t], x_recv.at[tp, x], (gr, fs, t))

    loop(0, per, exchange)

    def reduce_one(x):
        for j in range(1, n_tp):
            t = (tp + j) % n_tp
            settle(got.at[t, x], x_recv.at[t, x])

        def add(f):
            total = part[x, f, :, span(tp, wide)].astype(jnp.float32)
            for j in range(1, n_tp):
                total = total + got[(tp + j) % n_tp, x, f].astype(jnp.float32)
            summed[x, f] = total.astype(jnp.bfloat16)

        loop(0, n_fs, add)
        ret[fs, x] = summed[x, fs]

        def send(k):
            f = (fs + (k + n_fs // 2 - 1) % (n_fs - 1) + 1) % n_fs
            remote(summed.at[x, f], ret.at[fs, x], z_send, z_recv.at[fs], (gr, f, tp))

        loop(0, n_fs - 1, send)

    loop(0, per, reduce_one)
    loop(1, n_fs, lambda k: settle(ret.at[(fs + k) % n_fs], z_recv.at[(fs + k) % n_fs]))
    settle(summed.at[:, pl.ds(0, n_fs - 1)], z_send)
    for j in range(1, n_tp):
        t = (tp + j) % n_tp
        settle(part.at[:, :, :, span(t, wide)], x_send.at[t])


def body(sizes, prompt, norm_gain, gate_weight, up_weight, down_weight, routes, route_weight):
    n_gr, n_fs, n_tp = sizes
    gate_cast = (gate_weight * norm_gain[None, :, None]).astype(jnp.bfloat16)
    up_cast = (up_weight * norm_gain[None, :, None]).astype(jnp.bfloat16)
    down_cast = down_weight.astype(jnp.bfloat16)
    values = prompt.astype(jnp.float32)
    tok_count, wide = prompt.shape
    full_width = wide * n_tp
    squares = jnp.sum(values * values, axis=-1, keepdims=True)
    total_squares = lax.psum(squares, "tp")
    normed = (values * lax.rsqrt(total_squares / full_width + 1e-06)).astype(jnp.bfloat16)
    experts, blk, _ = gate_weight.shape
    per = experts // n_fs
    slots_all = experts * SLOT
    picks_flat = routes.reshape(-1)
    matches = picks_flat[:, None] == jnp.arange(experts, dtype=jnp.int32)[None, :]
    order = jnp.arange(2 * tok_count, dtype=jnp.int32)
    before = (order[None, :] < order[:, None]).astype(jnp.bfloat16)
    earlier = jnp.dot(before, matches.astype(jnp.bfloat16), preferred_element_type=jnp.float32)
    slot_of = jnp.sum(jnp.where(matches, earlier, 0.0), axis=1).astype(jnp.int32)
    target = (picks_flat * SLOT + slot_of).reshape(tok_count, 2)
    slot_ids = jnp.arange(slots_all, dtype=jnp.int32)[None, :]
    select_first = (target[:, 0:1] == slot_ids).astype(jnp.bfloat16)
    select_second = (target[:, 1:2] == slot_ids).astype(jnp.bfloat16)
    select_both = select_first + select_second
    outbound = jnp.einsum("ts,td->sd", select_both, normed, preferred_element_type=jnp.float32)
    outbound = outbound.astype(jnp.bfloat16).reshape(n_fs, per, SLOT, wide)

    any_spec = pl.BlockSpec(memory_space=pl.ANY)
    rows = n_gr * n_fs * blk
    bf16 = jnp.bfloat16
    dma = pltpu.SemaphoreType.DMA
    arrived, gate_new, up_new, down_new = pl.pallas_call(
        functools.partial(spread_kernel, sizes),
        out_shape=(
            jax.ShapeDtypeStruct((per, n_fs, SLOT, full_width), bf16),
            jax.ShapeDtypeStruct((per, rows, wide), bf16),
            jax.ShapeDtypeStruct((per, rows, wide), bf16),
            jax.ShapeDtypeStruct((per, rows // n_tp, full_width), bf16),
        ),
        in_specs=[any_spec] * 4,
        out_specs=(any_spec,) * 4,
        scratch_shapes=[
            pltpu.VMEM((per, SLOT, wide), bf16),
            pltpu.VMEM((3, per, blk, wide), bf16),
            dma(()),
            dma((n_fs,)),
            dma((n_tp,)),
            dma((n_tp,)),
            dma((3,)),
            dma((3, n_fs)),
            dma((3, n_gr)),
            dma((3, n_gr)),
            dma((4,)),
        ],
        compiler_params=pltpu.CompilerParams(collective_id=0, has_side_effects=True),
        name="spread",
    )(outbound, gate_cast, up_cast, down_cast)

    arrived = arrived.reshape(per, n_fs * SLOT, full_width)
    gate_pre = jnp.einsum("xcd,xdh->xch", arrived, gate_new, preferred_element_type=jnp.float32)
    up_pre = jnp.einsum("xcd,xdh->xch", arrived, up_new, preferred_element_type=jnp.float32)
    hidden = (jax.nn.silu(gate_pre) * up_pre).astype(bf16)
    partial_value = jnp.einsum("xch,xhd->xcd", hidden, down_new, preferred_element_type=jnp.float32)
    partial_value = partial_value.astype(bf16).reshape(per, n_fs, SLOT, full_width)

    vmem_spec = pl.BlockSpec(memory_space=pltpu.VMEM)
    returned = pl.pallas_call(
        functools.partial(return_kernel, sizes),
        out_shape=jax.ShapeDtypeStruct((n_fs, per, SLOT, wide), bf16),
        in_specs=[vmem_spec],
        out_specs=vmem_spec,
        scratch_shapes=[
            pltpu.VMEM((n_tp, per, n_fs, SLOT, wide), bf16),
            pltpu.VMEM((per, n_fs, SLOT, wide), bf16),
            dma((n_tp,)),
            dma((n_tp, per)),
            dma(()),
            dma((n_fs,)),
        ],
        compiler_params=pltpu.CompilerParams(collective_id=1, has_side_effects=True),
        name="give_back",
    )(partial_value)
    returned_flat = returned.reshape(slots_all, wide)
    pick_first = jnp.dot(select_first, returned_flat, preferred_element_type=jnp.float32)
    pick_second = jnp.dot(select_second, returned_flat, preferred_element_type=jnp.float32)
    mixed = route_weight[:, 0:1] * pick_first + route_weight[:, 1:2] * pick_second
    return (gate_new, up_new, down_new, mixed.astype(bf16))


def solution(mesh):
    sizes = (mesh.shape["gr"], mesh.shape["fs"], mesh.shape["tp"])
    return jax.shard_map(
        functools.partial(body, sizes),
        mesh=mesh,
        in_specs=(
            P(("gr", "fs"), "tp"),
            P(("gr", "fs")),
            P(None, ("gr", "fs"), "tp"),
            P(None, ("gr", "fs"), "tp"),
            P(None, ("gr", "fs"), "tp"),
            P(("gr", "fs"), None),
            P(("gr", "fs"), None),
        ),
        out_specs=(
            P("fs", None, "tp"),
            P("fs", None, "tp"),
            P("fs", "tp", None),
            P(("gr", "fs"), "tp"),
        ),
        check_vma=False,
    )
```
